32 devices in a mesh: ep: 16 (over z, y, x), tp: 2 (over core).
Axes of the slice: x: 2, y: 2, z: 4, core: 2. Of those that a mesh axis runs over, the one named last changes fastest.
Arguments:
- tokens: bfloat16 [128, 2048], P('ep'), may hold values from -6 to 6
- mixer_norm_gain: float32 [2048], replicated, may hold values from 0.1 to 1.9
- gate_projection_weight: bfloat16 [2048, 2, 2048], P(None, 'tp', 'ep'), may hold values from -0.125 to 0.125
- value_projection_weight: bfloat16 [2048, 2, 2048], P(None, 'tp', 'ep'), may hold values from -0.125 to 0.125
- input_projection_weight: bfloat16 [2048, 1024], P(None, 'tp'), may hold values from -0.125 to 0.125
- output_projection_weight: bfloat16 [2048, 1024], P(None, 'tp'), may hold values from -0.125 to 0.125
- step_projection_weight: bfloat16 [2048, 64], P(None, 'tp'), may hold values from -0.125 to 0.125
- head_step_bias: float32 [64], P('tp'), may hold values from -1 to 1
- head_decay_rate: float32 [64], P('tp'), may hold values from 0.02 to 3
- extra_log_decay: float32 [128, 64], P('ep', 'tp'), may hold values from -0.7 to 0
- value_taps: float32 [4, 4096], P(None, 'tp'), may hold values from -3 to 3
- input_taps: float32 [4, 1024], P(None, 'tp'), may hold values from -3 to 3
- output_taps: float32 [4, 1024], P(None, 'tp'), may hold values from -3 to 3
- prior_values: bfloat16 [128, 3, 4096], P('ep', None, 'tp'), may hold values from -6 to 6
- prior_input_maps: bfloat16 [128, 3, 1024], P('ep', None, 'tp'), may hold values from -6 to 6
- prior_output_maps: bfloat16 [128, 3, 1024], P('ep', None, 'tp'), may hold values from -6 to 6
- head_skip_gain: float32 [64], P('tp'), may hold values from 0.5 to 1.5
- group_norm_gain: float32 [4096], P('tp'), may hold values from 0.1 to 1.9
- mixer_output_weight: bfloat16 [4096, 2048], P('tp', 'ep'), may hold values from -0.09375 to 0.09375
- recurrent_state: float32 [128, 64, 64, 128], P('ep', 'tp'), may hold values from -6 to 6
- expert_norm_gain: float32 [2048], replicated, may hold values from 0.1 to 1.9
- routes: int32 [128, 6], P('ep'), may hold values from 0 to 15, all different within a row; in each aligned block of 8 rows (0 to 7, 8 to 15, ...) at most 4 rows name the same one
- chosen_expert_weight: float32 [128, 6], P('ep'), may hold values from 0.2 to 1
- routed_gate_weight: bfloat16 [16, 2048, 512], P('ep', None, 'tp'), may hold values from -0.125 to 0.125
- routed_up_weight: bfloat16 [16, 2048, 512], P('ep', None, 'tp'), may hold values from -0.125 to 0.125
- routed_down_weight: bfloat16 [16, 512, 2048], P('ep', 'tp'), may hold values from -0.25 to 0.25
- common_gate_weight: bfloat16 [2048, 512], P(None, 'tp'), may hold values from -0.125 to 0.125
- common_up_weight: bfloat16 [2048, 512], P(None, 'tp'), may hold values from -0.125 to 0.125
- common_down_weight: bfloat16 [512, 2048], P('tp'), may hold values from -0.25 to 0.25
Outputs:
- result: bfloat16 [128, 2048], P('ep')
- state_next: float32 [128, 64, 64, 128], P('ep', 'tp')
- next_value: bfloat16 [128, 3, 4096], P('ep', None, 'tp')
- next_input: bfloat16 [128, 3, 1024], P('ep', None, 'tp')
- next_output: bfloat16 [128, 3, 1024], P('ep', None, 'tp')
The draws below stay inside these ranges and needn't reach their ends.
Inputs may be any that keep to these rules, and one draw needn't show every extreme that they name: `routes`: the 6 experts of a row differ; among the rows of one device (aligned blocks of 8 rows) no expert is named more than 4 times.
All inputs are finite; a program needn't handle non-finite values.
Results may differ from the reference program's by a relative error of at most 0.015.
Values may be sent and summed in bfloat16 or wider, within the bound.
No kernel may reach another device: no remote copies, remote signals or barrier semaphores. Data moves between devices by JAX's collectives and lax.ppermute only.
A program may use at most 128 MiB of HBM per device.

```python
import math
import jax
import jax.numpy as jnp
import numpy as np
from jax import lax

D = 2048
D_INNER = 4096
HEAD = 64
MIXER_HEADS = 64
STATE = 128
GROUPS = 8
CONV = 4
FE = 512
FS = 512
TOPK = 6
EXPERTS = 16
SEQ_DEV = 8
SEQUENCE_COUNT = 128
CAP = 4
HALF = 2048
N_EP = 16
N_TP = 2


def shard_levels(stream_key, dims, pieces, least, top_value):
    def one(dim, blocks):
        heights = jax.random.uniform(jax.random.fold_in(jax.random.fold_in(stream_key, 6), dim), (blocks,), jnp.float32, least / len(pieces), top_value / len(pieces))
        return jnp.repeat(jnp.exp(heights), dims[dim] // blocks).reshape((-1,) + (1,) * (len(dims) - dim - 1))

    level = one(*pieces[0])
    for cut in pieces[1:]:
        level = level * one(*cut)
    return level


def deal_out(rng, own, number, rows, amount, top, reach, slope):
    order = jax.random.permutation(rng, amount)
    crowded, ordinary = load_shares(amount, rows * top, reach, slope, True), load_shares(amount, rows * top, reach, slope, False)
    places = jnp.arange(amount)

    def named(sizes, offset_by):
        used = int((sizes > 0).sum())
        fixed = max(1, used // 4)
        passed = fixed + (places - fixed + offset_by * (used - fixed)) % max(1, amount - fixed)
        return jnp.zeros((amount,), jnp.int32).at[order[jnp.where(places < fixed, places, passed)]].set(jnp.asarray(sizes, jnp.int32))

    sizes = jnp.where(number % 4 == 0, named(crowded, number // 4), named(ordinary, number - number // 4 - 1))
    mixed = jax.random.permutation(jax.random.fold_in(own, 3), amount)
    donor, taker = mixed[0:amount // 2 * 2:2], mixed[1:amount // 2 * 2:2]
    margin = jnp.minimum(sizes[donor] - 1, reach - sizes[taker]) // 2
    margin = jnp.where((donor == order[0]) | (taker == order[0]) | (sizes[taker] == 0), 0, jnp.maximum(margin, 0))
    passed = jax.random.randint(jax.random.fold_in(own, 4), (amount // 2,), 0, 1 << 20) % (margin + 1)
    sizes = sizes.at[donor].add(-passed).at[taker].add(passed)
    items = jnp.searchsorted(jnp.cumsum(sizes), jnp.arange(rows * top), side="right").astype(jnp.int32)
    grid = items.reshape(top, rows).T
    grid = grid[jax.random.permutation(jax.random.fold_in(own, 1), rows)]
    offset_by = jax.random.randint(jax.random.fold_in(own, 2), (rows, 1), 0, top)
    return jnp.take_along_axis(grid, (jnp.arange(top)[None, :] + offset_by) % top, axis=1)


def load_shares(count, total, reach, slope, full):
    portions = [(1 << 20) // math.isqrt(standing ** slope) + 1 for standing in range(1, count + 1)]
    largest = reach if full else min(reach, max(-(-total // count), total * portions[0] // sum(portions)))
    least = 1 if total - largest >= count - 1 else 0
    given, surplus = [largest] + [least] * (count - 1), total - largest - least * (count - 1)
    while surplus > 0:
        free = [i for i in range(1, count) if given[i] < largest] or [i for i in range(1, count) if given[i] < reach]
        pool, left = sum([portions[i] for i in free]), surplus
        for i in free:
            addition = min(reach - given[i], max(1, left * portions[i] // pool), surplus)
            given[i] = given[i] + addition
            surplus = surplus - addition
    return np.array(given)


def gaussian(key, shape, spread, limit, cuts=(), kind=jnp.bfloat16):
    drawn = spread * jax.random.normal(key, shape, jnp.float32)
    if cuts:
        drawn = drawn * shard_levels(key, shape, cuts, -0.22, 0.18)
    return jnp.clip(drawn, -limit, limit).astype(kind)


def setup_inputs(seed: int = 0) -> dict:
    key_list = jax.random.split(jax.random.key(seed), 30)
    tokens = gaussian(key_list[0], (SEQUENCE_COUNT, D), 1.0, 6.0, ((0, 16),))
    mixer_norm_gain = jnp.clip(1.0 + 0.18 * jax.random.normal(key_list[1], (D,), jnp.float32), 0.1, 1.9)
    gate_projection_weight = gaussian(key_list[2], (D, N_TP, HALF), D ** -0.5, 0.125, ((1, 2), (2, 16)))
    value_projection_weight = gaussian(key_list[3], (D, N_TP, HALF), D ** -0.5, 0.125, ((1, 2), (2, 16)))
    input_projection_weight = gaussian(key_list[4], (D, GROUPS * STATE), D ** -0.5, 0.125, ((1, 2),))
    output_projection_weight = gaussian(key_list[5], (D, GROUPS * STATE), D ** -0.5, 0.125, ((1, 2),))
    step_projection_weight = gaussian(key_list[6], (D, MIXER_HEADS), D ** -0.5, 0.125, ((1, 2),))
    head_step_bias = jnp.clip(jax.random.uniform(key_list[7], (MIXER_HEADS,), jnp.float32, -1.0, 1.0) * shard_levels(key_list[7], (MIXER_HEADS,), ((0, 2),), -0.4, 0.0), -1.0, 1.0)
    head_decay_rate = jnp.clip(jnp.exp(math.log(3.0) - 5.0106353 * jax.random.uniform(key_list[8], (MIXER_HEADS,), jnp.float32) ** shard_levels(key_list[8], (MIXER_HEADS,), ((0, 2),), -0.2, 0.2)), 0.02, 3.0)
    extra_log_decay = jnp.clip(-0.7 + 0.7 * jax.random.uniform(key_list[9], (SEQUENCE_COUNT, MIXER_HEADS), jnp.float32) ** shard_levels(key_list[9], (SEQUENCE_COUNT, MIXER_HEADS), ((0, 16), (1, 2)), -0.2, 0.2), -0.7, 0.0)
    value_taps = gaussian(key_list[10], (CONV, D_INNER), 0.5, 3.0, ((1, 2),), jnp.float32)
    input_taps = gaussian(key_list[11], (CONV, GROUPS * STATE), 0.5, 3.0, ((1, 2),), jnp.float32)
    output_taps = gaussian(key_list[12], (CONV, GROUPS * STATE), 0.5, 3.0, ((1, 2),), jnp.float32)
    prior_values = gaussian(key_list[13], (SEQUENCE_COUNT, CONV - 1, D_INNER), 1.0, 6.0, ((0, 16), (2, 2)))
    prior_input_maps = gaussian(key_list[14], (SEQUENCE_COUNT, CONV - 1, GROUPS * STATE), 1.0, 6.0, ((0, 16), (2, 2)))
    prior_output_maps = gaussian(key_list[15], (SEQUENCE_COUNT, CONV - 1, GROUPS * STATE), 1.0, 6.0, ((0, 16), (2, 2)))
    head_skip_gain = jnp.clip(0.5 + 1.0 * jax.random.uniform(key_list[16], (MIXER_HEADS,), jnp.float32) ** shard_levels(key_list[16], (MIXER_HEADS,), ((0, 2),), -0.2, 0.2), 0.5, 1.5)
    group_norm_gain = jnp.clip(1.0 + 0.18 * jax.random.normal(key_list[17], (D_INNER,), jnp.float32), 0.1, 1.9)
    mixer_output_weight = gaussian(key_list[18], (D_INNER, D), D_INNER ** -0.5, 0.09375, ((0, 2), (1, 16)))
    recurrent_state = gaussian(key_list[19], (SEQUENCE_COUNT, MIXER_HEADS, HEAD, STATE), 1.0, 6.0, ((0, 16), (1, 2)), jnp.float32)
    expert_norm_gain = jnp.clip(1.0 + 0.18 * jax.random.normal(key_list[20], (D,), jnp.float32), 0.1, 1.9)
    routes_keys = jax.random.split(jax.random.fold_in(key_list[21], 1), SEQUENCE_COUNT // SEQ_DEV)
    routes_turns = jax.random.permutation(jax.random.fold_in(key_list[21], 3), SEQUENCE_COUNT // SEQ_DEV)
    routes = jax.vmap(lambda own, number: deal_out(jax.random.fold_in(key_list[21], 2), own, number, SEQ_DEV, EXPERTS, TOPK, CAP, 1))(routes_keys, routes_turns).reshape((SEQUENCE_COUNT, TOPK))
    chosen_expert_weight = jnp.clip(0.2 + 0.8 * jax.random.uniform(key_list[22], (SEQUENCE_COUNT, TOPK), jnp.float32) ** shard_levels(key_list[22], (SEQUENCE_COUNT, TOPK), ((0, 16),), -0.2, 0.2), 0.2, 1.0)
    routed_gate_weight = gaussian(key_list[23], (EXPERTS, D, FE), D ** -0.5, 0.125, ((0, 16), (2, 2)))
    routed_up_weight = gaussian(key_list[24], (EXPERTS, D, FE), D ** -0.5, 0.125, ((0, 16), (2, 2)))
    routed_down_weight = gaussian(key_list[25], (EXPERTS, FE, D), FE ** -0.5, 0.25, ((0, 16), (1, 2)))
    common_gate_weight = gaussian(key_list[26], (D, FS), D ** -0.5, 0.125, ((1, 2),))
    common_up_weight = gaussian(key_list[27], (D, FS), D ** -0.5, 0.125, ((1, 2),))
    common_down_weight = gaussian(key_list[28], (FS, D), FS ** -0.5, 0.25, ((0, 2),))
    return dict(tokens=tokens, mixer_norm_gain=mixer_norm_gain, gate_projection_weight=gate_projection_weight, value_projection_weight=value_projection_weight, input_projection_weight=input_projection_weight, output_projection_weight=output_projection_weight, step_projection_weight=step_projection_weight, head_step_bias=head_step_bias, head_decay_rate=head_decay_rate, extra_log_decay=extra_log_decay, value_taps=value_taps, input_taps=input_taps, output_taps=output_taps, prior_values=prior_values, prior_input_maps=prior_input_maps, prior_output_maps=prior_output_maps, head_skip_gain=head_skip_gain, group_norm_gain=group_norm_gain, mixer_output_weight=mixer_output_weight, recurrent_state=recurrent_state, expert_norm_gain=expert_norm_gain, routes=routes, chosen_expert_weight=chosen_expert_weight, routed_gate_weight=routed_gate_weight, routed_up_weight=routed_up_weight, routed_down_weight=routed_down_weight, common_gate_weight=common_gate_weight, common_up_weight=common_up_weight, common_down_weight=common_down_weight)


EPSILON = 1e-06

def rms_scale(values, gain_vec):
    values = values.astype(jnp.float32)
    return values * lax.rsqrt(lax.optimization_barrier(jnp.mean(values * values, axis=-1, keepdims=True)) + EPSILON) * gain_vec

def short_conv(past_rows, fresh_row, weight):
    window = jnp.concatenate([past_rows, fresh_row[:, None, :]], axis=1)
    summed = window[:, 0].astype(jnp.float32) * weight[0]
    for offset in range(1, window.shape[1]):
        summed = summed + window[:, offset].astype(jnp.float32) * weight[offset]
    return (jax.nn.silu(summed), window[:, 1:])

def state_step(state_prev, value_conv, input_conv, output_conv, timestep_size, step_decay, head_skip_gain):
    batch_rows, head_count, head_size, state_size = state_prev.shape
    per_group = head_count // (input_conv.shape[1] // state_size)
    value_heads = value_conv.reshape(batch_rows, head_count, head_size)
    input_heads = jnp.repeat(input_conv.reshape(batch_rows, -1, state_size), per_group, axis=1)
    output_heads = jnp.repeat(output_conv.reshape(batch_rows, -1, state_size), per_group, axis=1)
    state_next = step_decay[:, :, None, None] * state_prev + (timestep_size[:, :, None] * value_heads)[:, :, :, None] * input_heads[:, :, None, :]
    mixed_heads = lax.optimization_barrier(jnp.sum(state_next * output_heads[:, :, None, :], axis=-1)) + head_skip_gain[None, :, None] * value_heads
    return (state_next, mixed_heads.reshape(batch_rows, -1))

def gated_norm(mixed_flat, gate_rows, group_norm_gain, group_width):
    gated_rows = mixed_flat * jax.nn.silu(gate_rows.astype(jnp.float32))
    grouped = gated_rows.reshape(gated_rows.shape[0], -1, group_width)
    grouped = grouped * lax.rsqrt(lax.optimization_barrier(jnp.mean(grouped * grouped, axis=-1, keepdims=True)) + EPSILON)
    return (grouped.reshape(gated_rows.shape[0], -1) * group_norm_gain).astype(jnp.bfloat16)

def half_sum(left_rows, right_matrix, halves):
    span_width = left_rows.shape[1] // halves
    summed = jnp.zeros((left_rows.shape[0], right_matrix.shape[1]), jnp.float32)
    for half_index in range(halves):
        partial_value = jnp.dot(left_rows[:, half_index * span_width:(half_index + 1) * span_width], right_matrix[half_index * span_width:(half_index + 1) * span_width], preferred_element_type=jnp.float32)
        rounded = lax.optimization_barrier(partial_value.astype(jnp.bfloat16))
        summed = summed + rounded.astype(jnp.float32)
    return summed

def reference(tokens, mixer_norm_gain, gate_projection_weight, value_projection_weight, input_projection_weight, output_projection_weight, step_projection_weight, head_step_bias, head_decay_rate, extra_log_decay, value_taps, input_taps, output_taps, prior_values, prior_input_maps, prior_output_maps, head_skip_gain, group_norm_gain, mixer_output_weight, recurrent_state, expert_norm_gain, routes, chosen_expert_weight, routed_gate_weight, routed_up_weight, routed_down_weight, common_gate_weight, common_up_weight, common_down_weight):
    normed = rms_scale(tokens, mixer_norm_gain).astype(jnp.bfloat16)
    gate_rows = jnp.dot(normed, gate_projection_weight.reshape(D, D_INNER), preferred_element_type=jnp.float32).astype(jnp.bfloat16)
    value_rows = jnp.dot(normed, value_projection_weight.reshape(D, D_INNER), preferred_element_type=jnp.float32).astype(jnp.bfloat16)
    input_rows = jnp.dot(normed, input_projection_weight, preferred_element_type=jnp.float32).astype(jnp.bfloat16)
    output_rows = jnp.dot(normed, output_projection_weight, preferred_element_type=jnp.float32).astype(jnp.bfloat16)
    step_raw = jnp.dot(normed, step_projection_weight, preferred_element_type=jnp.float32)
    value_conv, next_value = short_conv(prior_values, value_rows, value_taps)
    input_conv, next_input = short_conv(prior_input_maps, input_rows, input_taps)
    output_conv, next_output = short_conv(prior_output_maps, output_rows, output_taps)
    timestep_size = jax.nn.softplus(step_raw + head_step_bias)
    step_decay = jnp.exp(-timestep_size * head_decay_rate + extra_log_decay)
    state_next, mixed_flat = state_step(recurrent_state, value_conv, input_conv, output_conv, timestep_size, step_decay, head_skip_gain)
    mixer_rows = gated_norm(mixed_flat, gate_rows, group_norm_gain, D_INNER // GROUPS)
    mixed_out = half_sum(mixer_rows, mixer_output_weight, N_TP).astype(jnp.bfloat16)
    stream = (tokens.astype(jnp.float32) + mixed_out.astype(jnp.float32)).astype(jnp.bfloat16)
    ffn_rows = rms_scale(stream, expert_norm_gain).astype(jnp.bfloat16)
    shared_hidden = (jax.nn.silu(jnp.dot(ffn_rows, common_gate_weight, preferred_element_type=jnp.float32)) * jnp.dot(ffn_rows, common_up_weight, preferred_element_type=jnp.float32)).astype(jnp.bfloat16)
    shared_out = half_sum(shared_hidden, common_down_weight, N_TP)
    flat_routes = routes.reshape(N_EP, SEQ_DEV * TOPK)
    expert_ids = jnp.arange(EXPERTS, dtype=jnp.int32)
    onehot = (flat_routes[:, :, None] == expert_ids[None, None, :]).astype(jnp.int32)
    slot_ids = lax.optimization_barrier(jnp.sum((jnp.cumsum(onehot, axis=1) - onehot) * onehot, axis=2)).astype(jnp.int32)
    device_ids = jnp.broadcast_to(jnp.arange(N_EP, dtype=jnp.int32)[:, None], flat_routes.shape)
    token_ids = device_ids * SEQ_DEV + jnp.broadcast_to(jnp.arange(SEQ_DEV * TOPK, dtype=jnp.int32)[None, :] // TOPK, flat_routes.shape)
    slot_table = jnp.full((EXPERTS, N_EP, CAP), SEQUENCE_COUNT, jnp.int32).at[flat_routes, device_ids, slot_ids].set(token_ids)
    padded = jnp.concatenate([ffn_rows, jnp.zeros((1, D), jnp.bfloat16)], axis=0)

    def per_expert(operands):
        index_table, gate_mat, up_mat, down_mat = operands
        picked_rows = padded[index_table.reshape(-1)]
        hidden = (jax.nn.silu(jnp.dot(picked_rows, gate_mat, preferred_element_type=jnp.float32)) * jnp.dot(picked_rows, up_mat, preferred_element_type=jnp.float32)).astype(jnp.bfloat16)
        return half_sum(hidden, down_mat, N_TP).astype(jnp.bfloat16).reshape(N_EP, CAP, D)
    expert_out = lax.map(per_expert, (slot_table, routed_gate_weight, routed_up_weight, routed_down_weight))
    picked = expert_out[flat_routes, device_ids, slot_ids].astype(jnp.float32)
    weighted = picked * chosen_expert_weight.reshape(N_EP, SEQ_DEV * TOPK)[:, :, None]
    routed = lax.optimization_barrier(jnp.sum(weighted.reshape(SEQUENCE_COUNT, TOPK, D), axis=1))
    result = (stream.astype(jnp.float32) + shared_out + routed).astype(jnp.bfloat16)
    return (result, state_next, next_value, next_input, next_output)
```

```python
import jax
import jax.numpy as jnp
from jax import lax
from jax.sharding import PartitionSpec as P

GROUP_COUNT = 8
EPSILON = 1e-06
BF = jnp.bfloat16
F32 = jnp.float32


def dotf(a, b):
    return jnp.dot(a, b, preferred_element_type=F32)


def rms_rows(rows):
    return lax.rsqrt(jnp.mean(rows * rows, axis=-1, keepdims=True) + EPSILON)


def conv_rows(past_rows, fresh_row, taps):
    summed = fresh_row.astype(F32) * taps[-1]
    for offset in range(past_rows.shape[1]):
        summed = summed + past_rows[:, offset].astype(F32) * taps[offset]
    return jax.nn.silu(summed)


def shards(
    tokens,
    mixer_norm_gain,
    gate_projection_weight,
    value_projection_weight,
    input_projection_weight,
    output_projection_weight,
    step_projection_weight,
    head_step_bias,
    head_decay_rate,
    extra_log_decay,
    value_taps,
    input_taps,
    output_taps,
    prior_values,
    prior_input_maps,
    prior_output_maps,
    head_skip_gain,
    group_norm_gain,
    mixer_output_weight,
    recurrent_state,
    expert_norm_gain,
    routes,
    chosen_expert_weight,
    routed_gate_weight,
    routed_up_weight,
    routed_down_weight,
    common_gate_weight,
    common_up_weight,
    common_down_weight,
):
    seqs, width = tokens.shape
    n_ep = lax.axis_size("ep")
    n_tp = lax.axis_size("tp")
    ep = lax.axis_index("ep")
    tp = lax.axis_index("tp")
    total = n_ep * seqs
    half = width // n_tp
    topk = routes.shape[1]
    heads, head_size, state_size = recurrent_state.shape[1:]
    channels = heads * head_size
    groups = input_projection_weight.shape[1] // state_size
    per_group = heads // groups

    def to_all(rows):
        wide = jnp.broadcast_to(rows[None], (n_ep,) + rows.shape)
        return lax.all_to_all(wide, "ep", split_axis=0, concat_axis=0, tiled=True)

    def swap(rows):
        return lax.ppermute(rows, "tp", [(i, (i + 1) % n_tp) for i in range(n_tp)])

    own_half = lax.dynamic_slice_in_dim(tokens, tp * half, half, 1)
    route_cols = jnp.pad(routes.astype(BF), ((0, 0), (0, 128 - topk)))
    halves = to_all(jnp.concatenate([own_half, route_cols], axis=1))
    all_routes = halves[:, :, half : half + topk].reshape(total, topk).astype(jnp.int32)
    tokens_all = lax.all_gather(
        halves[:, :, :half].reshape(total, half), "tp", axis=1, tiled=True
    ).astype(F32)

    own = tokens.astype(F32)
    normed = (own * rms_rows(own) * mixer_norm_gain).astype(BF)
    input_rows = dotf(normed, input_projection_weight).astype(BF)
    output_rows = dotf(normed, output_projection_weight).astype(BF)
    step_raw = dotf(normed, step_projection_weight)
    input_conv = conv_rows(prior_input_maps, input_rows, input_taps)
    output_conv = conv_rows(prior_output_maps, output_rows, output_taps)
    step_size = jax.nn.softplus(step_raw + head_step_bias)
    decay = jnp.exp(-step_size * head_decay_rate + extra_log_decay)
    input_g = input_conv.reshape(seqs, groups, state_size)
    output_g = output_conv.reshape(seqs, groups, state_size)
    input_heads = jnp.repeat(input_g, per_group, axis=1)
    output_heads = jnp.repeat(output_g, per_group, axis=1)
    map_dot = jnp.repeat(jnp.sum(input_g * output_g, axis=-1), per_group, axis=1)
    read_out = jnp.sum(recurrent_state * output_heads[:, :, None, :], axis=-1)
    base_rows = (decay[:, :, None] * read_out).reshape(seqs, channels)
    slope = step_size * map_dot + head_skip_gain

    def widen(per_head):
        return jnp.broadcast_to(per_head[:, :, None], (seqs, heads, head_size)).reshape(
            seqs, channels
        )

    slope_rows = widen(slope)

    normed_all = (tokens_all * rms_rows(tokens_all) * mixer_norm_gain).astype(BF)
    both = jnp.concatenate(
        [
            gate_projection_weight.reshape(width, -1),
            value_projection_weight.reshape(width, -1),
        ],
        axis=1,
    )
    piece = both.shape[1] // 2
    projected = dotf(normed_all, both).astype(BF).reshape(n_ep, seqs, 2 * piece)
    returned = lax.all_to_all(projected, "ep", split_axis=0, concat_axis=0, tiled=True)
    gate_rows = jnp.swapaxes(returned[:, :, :piece], 0, 1).reshape(seqs, channels)
    value_rows = jnp.swapaxes(returned[:, :, piece:], 0, 1).reshape(seqs, channels)

    value_conv = conv_rows(prior_values, value_rows, value_taps)
    mixed_flat = base_rows + slope_rows * value_conv
    gated = (mixed_flat * jax.nn.silu(gate_rows.astype(F32))).reshape(seqs, groups, -1)
    mixer_rows = (
        (gated * rms_rows(gated)).reshape(seqs, channels) * group_norm_gain
    ).astype(BF)

    rows_all = to_all(mixer_rows).reshape(total, channels)
    partial = dotf(rows_all, mixer_output_weight).astype(BF)
    block = total // n_tp
    mine = lax.dynamic_slice_in_dim(partial, tp * block, block, 0)
    other = lax.dynamic_slice_in_dim(partial, (n_tp - 1 - tp) * block, block, 0)
    summed = (mine.astype(F32) + swap(other).astype(F32)).astype(BF)
    mixed_all = lax.all_gather(to_all(summed), "tp", axis=1, tiled=True)
    mixed_all = jnp.swapaxes(mixed_all, 0, 1).reshape(total, width)

    stream_all = (tokens_all + mixed_all.astype(F32)).astype(BF)
    stream32 = stream_all.astype(F32)
    ffn_all = (stream32 * rms_rows(stream32) * expert_norm_gain).astype(BF)

    exp_local = routed_gate_weight.shape[0]
    experts = exp_local * n_ep
    cap = (seqs * topk + experts - 1) // experts + 1
    slots = jnp.arange(cap, dtype=jnp.int32)

    def dispatch(local):
        named = jnp.any(all_routes == ep * exp_local + local, axis=1).reshape(n_ep, seqs)
        place = jnp.cumsum(named.astype(jnp.int32), axis=1) - 1
        pick = named[:, None, :] & (place[:, None, :] == slots[None, :, None])
        eye = jnp.arange(n_ep)[:, None] == jnp.arange(n_ep)[None, :]
        return (
            (pick[:, :, None, :] & eye[:, None, :, None]).reshape(n_ep * cap, total).astype(BF)
        )

    outs = []
    for local in range(exp_local):
        picked = dotf(dispatch(local), ffn_all).astype(BF)
        hidden = (
            jax.nn.silu(dotf(picked, routed_gate_weight[local]))
            * dotf(picked, routed_up_weight[local])
        ).astype(BF)
        outs.append(dotf(hidden, routed_down_weight[local]).astype(BF))
    sent = jnp.stack([o.reshape(n_ep, cap, width) for o in outs], axis=1)
    back = lax.all_to_all(sent, "ep", split_axis=0, concat_axis=0, tiled=True)
    back = back.reshape(experts * cap, width)

    stream_own = lax.dynamic_slice_in_dim(stream_all, ep * seqs, seqs, 0)
    ffn_own = lax.dynamic_slice_in_dim(ffn_all, ep * seqs, seqs, 0)
    shared_hidden = (
        jax.nn.silu(dotf(ffn_own, common_gate_weight)) * dotf(ffn_own, common_up_weight)
    ).astype(BF)
    shared_part = dotf(shared_hidden, common_down_weight)
    expert_ids = jnp.arange(experts, dtype=jnp.int32)
    hit = routes[:, :, None] == expert_ids
    weight_of = jnp.sum(jnp.where(hit, chosen_expert_weight[:, :, None], 0.0), axis=1)
    named = jnp.any(hit, axis=1).astype(jnp.int32)
    place = jnp.cumsum(named, axis=0) - named
    combine = jnp.where(
        place[:, :, None] == slots[None, None, :], weight_of[:, :, None], 0.0
    ).reshape(seqs, experts * cap)
    routed_part = jnp.dot(combine, back.astype(F32), precision=lax.Precision.HIGHEST)
    part = (shared_part + routed_part).astype(BF)
    other_part = swap(part)
    result = (
        stream_own.astype(F32) + (part.astype(F32) + other_part.astype(F32))
    ).astype(BF)

    state_next = (
        decay[:, :, None, None] * recurrent_state
        + (step_size[:, :, None] * value_conv.reshape(seqs, heads, head_size))[..., None]
        * input_heads[:, :, None, :]
    )

    def shifted(past, fresh):
        return jnp.concatenate([past[:, 1:], fresh[:, None]], axis=1)

    return (
        result,
        state_next,
        shifted(prior_values, value_rows),
        shifted(prior_input_maps, input_rows),
        shifted(prior_output_maps, output_rows),
    )


def solution(mesh):
    return jax.shard_map(
        shards,
        mesh=mesh,
        in_specs=(
            P("ep", None),
            P(),
            P(None, "tp", "ep"),
            P(None, "tp", "ep"),
            P(None, "tp"),
            P(None, "tp"),
            P(None, "tp"),
            P("tp"),
            P("tp"),
            P("ep", "tp"),
            P(None, "tp"),
            P(None, "tp"),
            P(None, "tp"),
            P("ep", None, "tp"),
            P("ep", None, "tp"),
            P("ep", None, "tp"),
            P("tp"),
            P("tp"),
            P("tp", "ep"),
            P("ep", "tp", None, None),
            P(),
            P("ep", None),
            P("ep", None),
            P("ep", None, "tp"),
            P("ep", None, "tp"),
            P("ep", "tp", None),
            P(None, "tp"),
            P(None, "tp"),
            P("tp", None),
        ),
        out_specs=(
            P("ep", None),
            P("ep", "tp", None, None),
            P("ep", None, "tp"),
            P("ep", None, "tp"),
            P("ep", None, "tp"),
        ),
        check_vma=False,
    )
```
